32 devices in a mesh: sp: 8 (over z, x), dp: 4 (over y, core).
Axes of the slice: x: 2, y: 2, z: 4, core: 2. Of those that a mesh axis runs over, the one named last changes fastest.
Arguments:
- queries: bfloat16 [16, 8, 512, 128], P('dp', None, 'sp'), may hold values from -6 to 6
- keys: bfloat16 [16, 8, 512, 128], P('dp', None, 'sp'), may hold values from -6 to 6
- values: bfloat16 [16, 8, 512, 128], P('dp', None, 'sp'), may hold values from -6 to 6
- input_gate: bfloat16 [16, 8, 512], P('dp', None, 'sp'), may hold values from -6 to 140
- forget_gate: bfloat16 [16, 8, 512], P('dp', None, 'sp'), may hold values from 0.5 to 11.5
- start_memory: float32 [16, 8, 128, 128], P('dp', None, 'sp'), may hold values from -6 to 6
- start_norm: float32 [16, 8, 128], P('dp', None, 'sp'), may hold values from -24 to 24
- start_level: float32 [16, 8], P('dp'), may hold values from 2 to 4
- head_gain: float32 [8, 128], replicated, may hold values from 0.1 to 1.9
- out_weight: bfloat16 [1024, 4096], P(None, 'dp'), may hold values from -0.1875 to 0.1875
Outputs:
- mixed: bfloat16 [16, 512, 4096], P('dp', 'sp')
The draws below stay inside these ranges and needn't reach their ends.
All inputs are finite; a program needn't handle non-finite values.
Results may differ from the reference program's by a relative error of at most 0.019.
Values may be sent and summed in bfloat16 or wider, within the bound.
No kernel may reach another device: no remote copies, remote signals or barrier semaphores. Data moves between devices by JAX's collectives and lax.ppermute only.
A program may use at most 64 MiB of HBM per device.

```python
import jax
import jax.numpy as jnp
from jax import lax

D = 4096
HEADS = 8
HD = 128
BLOCK = 64
SEG = 64
MIX = 1024
LEN = 512
BATCH = 16


def draw_input_gate(key, part):
    first, second, third = jax.random.split(key, 3)
    plain = jax.random.normal(first, (BATCH, HEADS, LEN), jnp.float32)
    result = jnp.clip(plain, -6.0, 6.0)
    return result.astype(jnp.bfloat16)


def draw_forget_gate(key, part):
    first, second, third = jax.random.split(key, 3)
    slow_share = 0.5
    slow = jax.random.bernoulli(first, slow_share, (BATCH, HEADS, 1))
    base = jnp.where(slow, jnp.log(LEN / 1.2), 3.5)
    spans = LEN // SEG
    factor = jnp.exp(jax.random.uniform(second, (BATCH, HEADS, spans), jnp.float32, -0.693, 0.693))
    factor = jnp.repeat(factor, SEG, axis=2)
    noise = 0.3 * jax.random.normal(third, (BATCH, HEADS, LEN), jnp.float32)
    result = jnp.clip(base - jnp.log(factor) + noise, 0.5, 11.5)
    return result.astype(jnp.bfloat16)


def block_levels(rng, extent, pieces, low, top_value):
    level, own = 1.0, jax.random.fold_in(rng, 6)
    for dim, parts in pieces:
        steps = jnp.exp(jax.random.uniform(jax.random.fold_in(own, dim), (parts,), jnp.float32, low / len(pieces), top_value / len(pieces)))
        level = level * jnp.repeat(steps, extent[dim] // parts).reshape([-1 if axis == dim else 1 for axis in range(len(extent))])
    return level


def centred(key, shape, spread, bound, shards=(), kind=jnp.bfloat16):
    values = jax.random.normal(key, shape, jnp.float32) * spread
    if len(shards) > 0:
        values = block_levels(key, shape, shards, -0.22, 0.18) * values
    return jnp.clip(values, min=-bound, max=bound).astype(kind)


def setup_inputs(seed: int = 0) -> dict:
    seeds = jax.random.split(jax.random.key(seed), 11)
    queries = centred(seeds[0], (BATCH, HEADS, LEN, HD), 1.0, 6.0, ((0, 4), (2, 8)))
    keys = centred(seeds[1], (BATCH, HEADS, LEN, HD), 1.0, 6.0, ((0, 4), (2, 8)))
    values = centred(seeds[2], (BATCH, HEADS, LEN, HD), 1.0, 6.0, ((0, 4), (2, 8)))
    input_gate = draw_input_gate(jax.random.fold_in(seeds[10], 71), 0)
    forget_gate = draw_forget_gate(jax.random.fold_in(seeds[10], 71), 0)
    start_memory = centred(seeds[5], (BATCH, HEADS, HD, HD), 1.0, 6.0, ((0, 4), (2, 8)), jnp.float32)
    start_norm = centred(seeds[6], (BATCH, HEADS, HD), 4.0, 24.0, ((0, 4), (2, 8)), jnp.float32)
    start_level = jnp.clip(2.0 + 2.0 * jax.random.uniform(seeds[7], (BATCH, HEADS), jnp.float32) ** block_levels(seeds[7], (BATCH, HEADS), ((0, 4),), -0.2, 0.2), 2.0, 4.0)
    head_gain = jnp.clip(1.0 + 0.18 * jax.random.normal(seeds[8], (HEADS, HD), jnp.float32), 0.1, 1.9)
    out_weight = centred(seeds[9], (MIX, D), MIX ** -0.5, 0.1875, ((1, 4),))
    return dict(queries=queries, keys=keys, values=values, input_gate=input_gate, forget_gate=forget_gate, start_memory=start_memory, start_norm=start_norm, start_level=start_level, head_gain=head_gain, out_weight=out_weight)


negative_fill = -1e30
highest = lax.Precision.HIGHEST


def cell_scan(query, key_in, value, input_pre, forget_pre, memory, normal, stabilizer):
    item_count, length, head_width = query.shape
    blocks = length // BLOCK
    factor = head_width ** -0.5

    def blocked(tensor):
        return jnp.moveaxis(tensor.reshape((item_count, blocks, BLOCK) + tensor.shape[2:]), 1, 0)

    inputs = (blocked(query), blocked(key_in), blocked(value),
              blocked(input_pre.astype(jnp.float32)), blocked(jax.nn.log_sigmoid(forget_pre.astype(jnp.float32))))
    causal = jnp.tril(jnp.ones((BLOCK, BLOCK), dtype=bool))

    def advance(state, block_data):
        memory, normal, stabilizer = state
        query_block, key_block, value_block, gate_in, gate_keep = block_data
        query_wide = query_block.astype(jnp.float32)
        key_wide = key_block.astype(jnp.float32)
        value_wide = value_block.astype(jnp.float32)
        scaled = query_wide * factor
        cumulative = jnp.cumsum(gate_keep, axis=-1)
        logits = jnp.where(causal, cumulative[:, :, None] - cumulative[:, None, :] + gate_in[:, None, :], negative_fill)
        carried = cumulative + stabilizer[:, None]
        running_max = jnp.maximum(carried, jnp.max(logits, axis=-1))
        raw = jnp.einsum('ptd,psd->pts', query_wide, key_wide, precision=highest) * factor
        scores = raw * jnp.exp(logits - running_max[..., None])
        rounded = scores.astype(jnp.bfloat16).astype(jnp.float32)
        carry_weight = jnp.exp(carried - running_max)
        numerator = jnp.einsum('pts,pse->pte', rounded, value_wide, precision=highest) + carry_weight[..., None] * jnp.einsum('ptd,pde->pte', scaled, memory, precision=highest)
        denominator = jnp.sum(scores, axis=-1) + carry_weight * jnp.einsum('ptd,pd->pt', scaled, normal, precision=highest)
        output = numerator / jnp.maximum(jnp.abs(denominator), 1.0)[..., None]
        block_total = cumulative[:, -1]
        weights_log = block_total[:, None] - cumulative + gate_in
        stabilizer_new = jnp.maximum(block_total + stabilizer, jnp.max(weights_log, axis=-1))
        weights = jnp.exp(weights_log - stabilizer_new[:, None])
        shrink = jnp.exp(block_total + stabilizer - stabilizer_new)
        weighted = key_wide * weights[..., None]
        packed = weighted.astype(jnp.bfloat16).astype(jnp.float32)
        memory_new = shrink[:, None, None] * memory + jnp.einsum('psd,pse->pde', packed, value_wide, precision=highest)
        normal_new = shrink[:, None] * normal + jnp.sum(weighted, axis=1)
        return (memory_new, normal_new, stabilizer_new), output

    start = (memory.astype(jnp.float32), normal.astype(jnp.float32), stabilizer.astype(jnp.float32))
    _, outputs = lax.scan(advance, start, inputs)
    return jnp.moveaxis(outputs, 0, 1).reshape(item_count, length, head_width).astype(jnp.bfloat16)


def normalize(hidden, gain):
    entries = hidden.astype(jnp.float32)
    return (entries * gain[:, None, :]).astype(jnp.bfloat16)


def reference(queries, keys, values, input_gate, forget_gate, start_memory, start_norm, start_level, head_gain, out_weight):
    batch, heads, length, head_width = queries.shape
    count = batch * heads
    hidden = cell_scan(queries.reshape(count, length, head_width), keys.reshape(count, length, head_width),
                       values.reshape(count, length, head_width), input_gate.reshape(count, length),
                       forget_gate.reshape(count, length), start_memory.reshape(count, head_width, head_width),
                       start_norm.reshape(count, head_width), start_level.reshape(count))
    normed = normalize(hidden.reshape(batch, heads, length, head_width), head_gain)
    flat_rows = normed.transpose(0, 2, 1, 3).reshape(batch * length, heads * head_width)
    mixed = jnp.dot(flat_rows, out_weight, preferred_element_type=jnp.float32).astype(jnp.bfloat16)
    return mixed.reshape(batch, length, out_weight.shape[1])
```

```python
import jax
import jax.numpy as jnp
from jax import lax
from jax.sharding import PartitionSpec as P


negative_fill = -1e30
highest = lax.Precision.HIGHEST
CHUNKS = 2


def send(tensor, axis, size, move):
    return lax.ppermute(tensor, axis, [(k, move(k)) for k in range(size)])


def gather_weight(weight, size):
    me = lax.axis_index("dp")
    width = weight.shape[1] // CHUNKS
    chunks = [weight[:, c * width : (c + 1) * width] for c in range(CHUNKS)]
    rounds = size // 2
    pieces = []
    for c in range(CHUNKS):
        pieces.append((me, c, chunks[c]))
    for c in range(CHUNKS):
        pieces.append((me ^ 1, c, send(chunks[c], "dp", size, lambda k: k ^ 1)))
    for step in range(1, rounds):
        for c in range(CHUNKS):
            far = send(chunks[c], "dp", size, lambda k: (k + 2 * step) % size)
            source = (me - 2 * step) % size
            pieces.append((source, c, far))
            pieces.append((source ^ 1, c, send(far, "dp", size, lambda k: k ^ 1)))
    return pieces, width


def gather_small(tensor, size):
    me = lax.axis_index("sp")
    whole = tensor[None]
    bit = 1
    while bit < size:
        other = send(whole, "sp", size, lambda k: k ^ bit)
        upper = (me & bit) != 0
        whole = jnp.concatenate(
            [jnp.where(upper, other, whole), jnp.where(upper, whole, other)], axis=0
        )
        bit *= 2
    return whole


def pick(tensor, index):
    return lax.dynamic_index_in_dim(tensor, index, 0, keepdims=False)


def cell(query, key_in, value, input_pre, forget_pre, memory, normal, level, size):
    count, length, head_width = query.shape
    rows = memory.shape[1]
    factor = head_width ** (-0.5)
    me = lax.axis_index("sp")
    side = me % 2
    pair = me // 2
    pairs = size // 2

    gate_in = input_pre.astype(jnp.float32)
    cumulative = jnp.cumsum(jax.nn.log_sigmoid(forget_pre.astype(jnp.float32)), axis=-1)
    total = cumulative[:, -1]
    weights_log = total[:, None] - cumulative + gate_in
    local_max = jnp.max(weights_log, axis=-1)
    weights = jnp.exp(weights_log - local_max[:, None])
    weighted = key_in.astype(jnp.float32) * weights[..., None]
    local_norm = jnp.sum(weighted, axis=1)
    small = jnp.concatenate(
        [local_norm, normal, total[:, None], local_max[:, None]], axis=1
    )
    gathered = gather_small(small, size)

    added = jnp.einsum(
        "psd,pse->pde", weighted.astype(jnp.bfloat16), value, preferred_element_type=jnp.float32
    ).astype(jnp.bfloat16)
    groups = added.reshape(count, pairs, 2, rows, head_width)
    even = groups[:, :, 0]
    odd = groups[:, :, 1]
    first = side == 0
    kept = jnp.where(first, even, odd)
    partner = send(jnp.where(first, odd, even), "sp", size, lambda k: k ^ 1)
    low = jnp.where(first, kept, partner).astype(jnp.float32)
    high = jnp.where(first, partner, kept).astype(jnp.float32)

    norms = gathered[:, :, :head_width]
    start_normal = jnp.moveaxis(
        gathered[:, :, head_width : head_width + rows], 0, 1
    ).reshape(count, head_width)
    totals = jnp.cumsum(gathered[:, :, head_width + rows], axis=0)
    own_level = gathered[:, :, head_width + rows + 1] - totals
    after = jnp.maximum(lax.cummax(own_level, axis=0), level[None])
    before = jnp.concatenate([level[None], after[:-1]], axis=0)
    even_before = before[0::2]
    odd_after = after[1::2]

    low_scale = jnp.exp(pick(own_level, 2 * pair) - pick(odd_after, pair))
    high_scale = jnp.exp(pick(own_level, 2 * pair + 1) - pick(odd_after, pair))
    both = (
        low_scale[:, None, None, None] * low + high_scale[:, None, None, None] * high
    ).astype(jnp.bfloat16)
    both = jnp.swapaxes(both, 0, 1)
    arrived = [pick(both, pair)]
    for step in range(1, pairs):
        arrived.append(
            send(
                pick(both, (pair + step) % pairs),
                "sp",
                size,
                lambda k: (k + 2 * step) % size,
            )
        )
    states = []
    for step in range(pairs):
        target = (pair + step) % pairs
        frame = pick(even_before, target)
        state = jnp.exp(level - frame)[:, None, None] * memory
        for back in range(pairs):
            source = (pair - back) % pairs
            scale = jnp.where(
                source < target, jnp.exp(jnp.minimum(pick(odd_after, source) - frame, 0.0)), 0.0
            )
            state = state + scale[:, None, None] * arrived[back].astype(jnp.float32)
        states.append(state.astype(jnp.bfloat16))
    returned = [states[0]]
    for step in range(1, pairs):
        returned.append(send(states[step], "sp", size, lambda k: (k + 2 * step) % size))
    stacked = jnp.stack(returned[::-1] + returned[::-1], axis=0)
    ordered = lax.dynamic_slice_in_dim(stacked, pairs - 1 - pair, pairs, axis=0)
    ordered = jnp.swapaxes(ordered, 0, 1)
    mid_after = pick(after, 2 * pair)
    mid = (
        jnp.exp(pick(even_before, pair) - mid_after)[:, None, None, None]
        * ordered.astype(jnp.float32)
        + jnp.exp(pick(own_level, 2 * pair) - mid_after)[:, None, None, None] * low
    ).astype(jnp.bfloat16)
    mine = jnp.where(first, ordered, mid)
    other = send(jnp.where(first, mid, ordered), "sp", size, lambda k: k ^ 1)
    state = jnp.stack(
        [jnp.where(first, mine, other), jnp.where(first, other, mine)], axis=2
    ).reshape(count, head_width, head_width)

    frame = pick(before, me)
    stabilizer = frame + pick(totals, me) - total
    blocks = jnp.arange(size)[:, None]
    shares = jnp.where(blocks < me, jnp.exp(jnp.minimum(own_level - frame[None], 0.0)), 0.0)
    norm_state = jnp.exp(level - frame)[:, None] * start_normal + jnp.sum(
        shares[..., None] * norms, axis=0
    )

    causal = jnp.tril(jnp.ones((length, length), dtype=bool))
    logits = jnp.where(
        causal,
        cumulative[:, :, None] - cumulative[:, None, :] + gate_in[:, None, :],
        negative_fill,
    )
    carried = cumulative + stabilizer[:, None]
    running_max = jnp.maximum(carried, jnp.max(logits, axis=-1))
    raw = (
        jnp.einsum("ptd,psd->pts", query, key_in, preferred_element_type=jnp.float32) * factor
    )
    scores = raw * jnp.exp(logits - running_max[..., None])
    carry_weight = jnp.exp(carried - running_max) * factor
    inner = jnp.einsum(
        "pts,pse->pte", scores.astype(jnp.bfloat16), value, preferred_element_type=jnp.float32
    )
    denominator = jnp.sum(scores, axis=-1) + carry_weight * jnp.sum(
        query.astype(jnp.float32) * norm_state[:, None, :], axis=-1
    )
    numerator = inner + carry_weight[..., None] * jnp.einsum(
        "ptd,pde->pte", query, state, preferred_element_type=jnp.float32
    )
    return (numerator / jnp.maximum(jnp.abs(denominator), 1.0)[..., None]).astype(jnp.bfloat16)


def on_device(
    queries,
    keys,
    values,
    input_gate,
    forget_gate,
    start_memory,
    start_norm,
    start_level,
    head_gain,
    out_weight,
):
    local_seqs, heads, tokens_here, head_width = queries.shape
    count = local_seqs * heads
    pieces, width = gather_weight(out_weight, lax.axis_size("dp"))

    def to_items(tensor):
        return tensor.reshape((count,) + tensor.shape[2:])

    hidden = cell(
        to_items(queries),
        to_items(keys),
        to_items(values),
        to_items(input_gate),
        to_items(forget_gate),
        to_items(start_memory),
        to_items(start_norm),
        start_level.reshape(count),
        lax.axis_size("sp"),
    ).reshape(local_seqs, heads, tokens_here, head_width)
    normed = (hidden.astype(jnp.float32) * head_gain[:, None, :]).astype(jnp.bfloat16)
    flat = jnp.swapaxes(normed, 1, 2).reshape(local_seqs, tokens_here, heads * head_width)
    mixed = jnp.zeros(
        (local_seqs, tokens_here, out_weight.shape[1] * lax.axis_size("dp")), jnp.bfloat16
    )
    for block, chunk, piece in pieces:
        part = jnp.einsum("stf,fc->stc", flat, piece, preferred_element_type=jnp.float32)
        mixed = lax.dynamic_update_slice(
            mixed,
            part.astype(jnp.bfloat16),
            (0, 0, block * out_weight.shape[1] + chunk * width),
        )
    return mixed


def solution(mesh):
    in_specs = (
        P("dp", None, "sp", None),
        P("dp", None, "sp", None),
        P("dp", None, "sp", None),
        P("dp", None, "sp"),
        P("dp", None, "sp"),
        P("dp", None, "sp", None),
        P("dp", None, "sp"),
        P("dp", None),
        P(),
        P(None, "dp"),
    )
    out_specs = P("dp", "sp", None)
    return jax.shard_map(
        on_device, mesh=mesh, in_specs=in_specs, out_specs=out_specs, check_vma=False
    )
```

```python
import jax
import jax.numpy as jnp
from jax import lax
from jax.sharding import PartitionSpec as P


negative_fill = -1e30
CHUNKS = 1


def send(tensor, axis, size, move):
    return lax.ppermute(tensor, axis, [(k, move(k)) for k in range(size)])


def gather_weight(weight, size):
    me = lax.axis_index("dp")
    width = weight.shape[1] // CHUNKS
    chunks = [weight[:, c * width : (c + 1) * width] for c in range(CHUNKS)]
    rounds = size // 2
    pieces = []
    for c in range(CHUNKS):
        pieces.append((me, c, chunks[c]))
    for c in range(CHUNKS):
        pieces.append((me ^ 1, c, send(chunks[c], "dp", size, lambda k: k ^ 1)))
    for step in range(1, rounds):
        for c in range(CHUNKS):
            far = send(chunks[c], "dp", size, lambda k: (k + 2 * step) % size)
            source = (me - 2 * step) % size
            pieces.append((source, c, far))
            pieces.append((source ^ 1, c, send(far, "dp", size, lambda k: k ^ 1)))
    return pieces, width


def gather_small(tensor, size):
    me = lax.axis_index("sp")
    whole = tensor[None]
    bit = 1
    while bit < size:
        other = send(whole, "sp", size, lambda k: k ^ bit)
        upper = (me & bit) != 0
        whole = jnp.concatenate(
            [jnp.where(upper, other, whole), jnp.where(upper, whole, other)], axis=0
        )
        bit *= 2
    return whole


def pick(tensor, index):
    return lax.dynamic_index_in_dim(tensor, index, 0, keepdims=False)


def cell(query, key_in, value, input_pre, forget_pre, memory, normal, level, size):
    count, length, head_width = query.shape
    rows = memory.shape[1]
    factor = head_width ** (-0.5)
    me = lax.axis_index("sp")
    side = me % 2
    pair = me // 2
    pairs = size // 2

    gate_in = input_pre.astype(jnp.float32)
    cumulative = jnp.cumsum(jax.nn.log_sigmoid(forget_pre.astype(jnp.float32)), axis=-1)
    total = cumulative[:, -1]
    weights_log = total[:, None] - cumulative + gate_in
    local_max = jnp.max(weights_log, axis=-1)
    weights = jnp.exp(weights_log - local_max[:, None])
    weighted = key_in.astype(jnp.float32) * weights[..., None]
    local_norm = jnp.sum(weighted, axis=1)
    small = jnp.concatenate(
        [local_norm, normal, total[:, None], local_max[:, None]], axis=1
    )
    added = jnp.einsum(
        "psd,pse->pde", weighted.astype(jnp.bfloat16), value, preferred_element_type=jnp.float32
    ).astype(jnp.bfloat16)
    groups = added.reshape(count, pairs, 2, rows, head_width)
    even = groups[:, :, 0]
    odd = groups[:, :, 1]
    first = side == 0
    kept = jnp.where(first, even, odd)
    given, small = lax.optimization_barrier((jnp.where(first, odd, even), small))
    partner = send(given, "sp", size, lambda k: k ^ 1)
    gathered = gather_small(small, size)
    low = jnp.where(first, kept, partner).astype(jnp.float32)
    high = jnp.where(first, partner, kept).astype(jnp.float32)

    norms = gathered[:, :, :head_width]
    start_normal = jnp.moveaxis(
        gathered[:, :, head_width : head_width + rows], 0, 1
    ).reshape(count, head_width)
    totals = jnp.cumsum(gathered[:, :, head_width + rows], axis=0)
    own_level = gathered[:, :, head_width + rows + 1] - totals
    after = jnp.maximum(lax.cummax(own_level, axis=0), level[None])
    before = jnp.concatenate([level[None], after[:-1]], axis=0)
    even_before = before[0::2]
    odd_after = after[1::2]

    low_scale = jnp.exp(pick(own_level, 2 * pair) - pick(odd_after, pair))
    high_scale = jnp.exp(pick(own_level, 2 * pair + 1) - pick(odd_after, pair))
    both = (
        low_scale[:, None, None, None] * low + high_scale[:, None, None, None] * high
    ).astype(jnp.bfloat16)
    both = jnp.swapaxes(both, 0, 1)
    arrived = [pick(both, pair)]
    for step in range(1, pairs):
        arrived.append(
            send(
                pick(both, (pair + step) % pairs),
                "sp",
                size,
                lambda k: (k + 2 * step) % size,
            )
        )
    states = []
    for step in range(pairs):
        target = (pair + step) % pairs
        frame = pick(even_before, target)
        state = jnp.exp(level - frame)[:, None, None] * memory
        for back in range(pairs):
            source = (pair - back) % pairs
            scale = jnp.where(
                source < target, jnp.exp(jnp.minimum(pick(odd_after, source) - frame, 0.0)), 0.0
            )
            state = state + scale[:, None, None] * arrived[back].astype(jnp.float32)
        states.append(state.astype(jnp.bfloat16))
    returned = [states[0]]
    for step in range(1, pairs):
        returned.append(send(states[step], "sp", size, lambda k: (k + 2 * step) % size))
    stacked = jnp.stack(returned[::-1] + returned[::-1], axis=0)
    ordered = lax.dynamic_slice_in_dim(stacked, pairs - 1 - pair, pairs, axis=0)
    ordered = jnp.swapaxes(ordered, 0, 1)
    mid_after = pick(after, 2 * pair)
    mid = (
        jnp.exp(pick(even_before, pair) - mid_after)[:, None, None, None]
        * ordered.astype(jnp.float32)
        + jnp.exp(pick(own_level, 2 * pair) - mid_after)[:, None, None, None] * low
    ).astype(jnp.bfloat16)
    mine = jnp.where(first, ordered, mid)
    other = send(jnp.where(first, mid, ordered), "sp", size, lambda k: k ^ 1)
    state = jnp.stack(
        [jnp.where(first, mine, other), jnp.where(first, other, mine)], axis=2
    ).reshape(count, head_width, head_width)

    frame = pick(before, me)
    stabilizer = frame + pick(totals, me) - total
    blocks = jnp.arange(size)[:, None]
    shares = jnp.where(blocks < me, jnp.exp(jnp.minimum(own_level - frame[None], 0.0)), 0.0)
    norm_state = jnp.exp(level - frame)[:, None] * start_normal + jnp.sum(
        shares[..., None] * norms, axis=0
    )

    causal = jnp.tril(jnp.ones((length, length), dtype=bool))
    logits = jnp.where(
        causal,
        cumulative[:, :, None] - cumulative[:, None, :] + gate_in[:, None, :],
        negative_fill,
    )
    carried = cumulative + stabilizer[:, None]
    running_max = jnp.maximum(carried, jnp.max(logits, axis=-1))
    raw = (
        jnp.einsum("ptd,psd->pts", query, key_in, preferred_element_type=jnp.float32) * factor
    )
    scores = raw * jnp.exp(logits - running_max[..., None])
    carry_weight = jnp.exp(carried - running_max) * factor
    inner = jnp.einsum(
        "pts,pse->pte", scores.astype(jnp.bfloat16), value, preferred_element_type=jnp.float32
    )
    denominator = jnp.sum(scores, axis=-1) + carry_weight * jnp.sum(
        query.astype(jnp.float32) * norm_state[:, None, :], axis=-1
    )
    numerator = inner + carry_weight[..., None] * jnp.einsum(
        "ptd,pde->pte", query, state, preferred_element_type=jnp.float32
    )
    return (numerator / jnp.maximum(jnp.abs(denominator), 1.0)[..., None]).astype(jnp.bfloat16)


def on_device(
    queries,
    keys,
    values,
    input_gate,
    forget_gate,
    start_memory,
    start_norm,
    start_level,
    head_gain,
    out_weight,
):
    local_seqs, heads, tokens_here, head_width = queries.shape
    count = local_seqs * heads
    pieces, width = gather_weight(out_weight, lax.axis_size("dp"))

    def to_items(tensor):
        return tensor.reshape((count,) + tensor.shape[2:])

    hidden = cell(
        to_items(queries),
        to_items(keys),
        to_items(values),
        to_items(input_gate),
        to_items(forget_gate),
        to_items(start_memory),
        to_items(start_norm),
        start_level.reshape(count),
        lax.axis_size("sp"),
    ).reshape(local_seqs, heads, tokens_here, head_width)
    normed = (hidden.astype(jnp.float32) * head_gain[:, None, :]).astype(jnp.bfloat16)
    flat = jnp.swapaxes(normed, 1, 2).reshape(local_seqs, tokens_here, heads * head_width)
    mixed = jnp.zeros(
        (local_seqs, tokens_here, out_weight.shape[1] * lax.axis_size("dp")), jnp.bfloat16
    )
    for block, chunk, piece in pieces:
        part = jnp.einsum("stf,fc->stc", flat, piece, preferred_element_type=jnp.float32)
        mixed = lax.dynamic_update_slice(
            mixed,
            part.astype(jnp.bfloat16),
            (0, 0, block * out_weight.shape[1] + chunk * width),
        )
    return mixed


def solution(mesh):
    in_specs = (
        P("dp", None, "sp", None),
        P("dp", None, "sp", None),
        P("dp", None, "sp", None),
        P("dp", None, "sp"),
        P("dp", None, "sp"),
        P("dp", None, "sp", None),
        P("dp", None, "sp"),
        P("dp", None),
        P(),
        P(None, "dp"),
    )
    out_specs = P("dp", "sp", None)

    return jax.shard_map(on_device, mesh=mesh, in_specs=in_specs, out_specs=out_specs, check_vma=False)
```

```python
import jax
import jax.numpy as jnp
from jax import lax
from jax.sharding import PartitionSpec as P


negative_fill = -1e30
CHUNKS = 1


def send(tensor, axis, size, move):
    return lax.ppermute(tensor, axis, [(k, move(k)) for k in range(size)])


def gather_weight(weight, size):
    me = lax.axis_index("dp")
    width = weight.shape[1] // CHUNKS
    chunks = [weight[:, c * width : (c + 1) * width] for c in range(CHUNKS)]
    rounds = size // 2
    pieces = []
    for c in range(CHUNKS):
        pieces.append((me, c, chunks[c]))
    for c in range(CHUNKS):
        pieces.append((me ^ 1, c, send(chunks[c], "dp", size, lambda k: k ^ 1)))
    for step in range(1, rounds):
        for c in range(CHUNKS):
            far = send(chunks[c], "dp", size, lambda k: (k + 2 * step) % size)
            source = (me - 2 * step) % size
            pieces.append((source, c, far))
            pieces.append((source ^ 1, c, send(far, "dp", size, lambda k: k ^ 1)))
    return pieces, width


def gather_small(tensor, size):
    me = lax.axis_index("sp")
    whole = tensor[None]
    bit = size // 2
    while bit > 0:
        other = send(whole, "sp", size, lambda k: k ^ bit)
        upper = (me & bit) != 0
        whole = jnp.stack(
            [jnp.where(upper, other, whole), jnp.where(upper, whole, other)], axis=1
        ).reshape((2 * whole.shape[0],) + whole.shape[1:])
        bit //= 2
    return whole


def pick(tensor, index):
    return lax.dynamic_index_in_dim(tensor, index, 0, keepdims=False)


def cell(query, key_in, value, input_pre, forget_pre, memory, normal, level, size):
    count, length, head_width = query.shape
    rows = memory.shape[1]
    factor = head_width ** (-0.5)
    me = lax.axis_index("sp")
    side = me % 2
    pair = me // 2
    pairs = size // 2

    gate_in = input_pre.astype(jnp.float32)
    cumulative = jnp.cumsum(jax.nn.log_sigmoid(forget_pre.astype(jnp.float32)), axis=-1)
    total = cumulative[:, -1]
    weights_log = total[:, None] - cumulative + gate_in
    local_max = jnp.max(weights_log, axis=-1)
    weights = jnp.exp(weights_log - local_max[:, None])
    weighted = key_in.astype(jnp.float32) * weights[..., None]
    local_norm = jnp.sum(weighted, axis=1)
    small = jnp.concatenate(
        [local_norm, normal, total[:, None], local_max[:, None]], axis=1
    )
    added = jnp.einsum(
        "psd,pse->pde", weighted.astype(jnp.bfloat16), value, preferred_element_type=jnp.float32
    ).astype(jnp.bfloat16)
    groups = added.reshape(count, pairs, 2, rows, head_width)
    even = groups[:, :, 0]
    odd = groups[:, :, 1]
    first = side == 0
    kept = jnp.where(first, even, odd)
    given, small = lax.optimization_barrier((jnp.where(first, odd, even), small))
    partner = send(given, "sp", size, lambda k: k ^ 1)
    gathered = gather_small(small, size)
    low = jnp.where(first, kept, partner).astype(jnp.float32)
    high = jnp.where(first, partner, kept).astype(jnp.float32)

    norms = gathered[:, :, :head_width]
    start_normal = jnp.moveaxis(
        gathered[:, :, head_width : head_width + rows], 0, 1
    ).reshape(count, head_width)
    totals = jnp.cumsum(gathered[:, :, head_width + rows], axis=0)
    own_level = gathered[:, :, head_width + rows + 1] - totals
    after = jnp.maximum(lax.cummax(own_level, axis=0), level[None])
    before = jnp.concatenate([level[None], after[:-1]], axis=0)
    even_before = before[0::2]
    odd_after = after[1::2]

    low_scale = jnp.exp(pick(own_level, 2 * pair) - pick(odd_after, pair))
    high_scale = jnp.exp(pick(own_level, 2 * pair + 1) - pick(odd_after, pair))
    both = (
        low_scale[:, None, None, None] * low + high_scale[:, None, None, None] * high
    ).astype(jnp.bfloat16)
    both = jnp.swapaxes(both, 0, 1)
    arrived = [pick(both, pair)]
    for step in range(1, pairs):
        arrived.append(
            send(
                pick(both, (pair + step) % pairs),
                "sp",
                size,
                lambda k: (k + 2 * step) % size,
            )
        )
    states = []
    for step in range(pairs):
        target = (pair + step) % pairs
        frame = pick(even_before, target)
        state = jnp.exp(level - frame)[:, None, None] * memory
        for back in range(pairs):
            source = (pair - back) % pairs
            scale = jnp.where(
                source < target, jnp.exp(jnp.minimum(pick(odd_after, source) - frame, 0.0)), 0.0
            )
            state = state + scale[:, None, None] * arrived[back].astype(jnp.float32)
        states.append(state.astype(jnp.bfloat16))
    returned = [states[0]]
    for step in range(1, pairs):
        returned.append(send(states[step], "sp", size, lambda k: (k + 2 * step) % size))
    stacked = jnp.stack(returned[::-1] + returned[::-1], axis=0)
    ordered = lax.dynamic_slice_in_dim(stacked, pairs - 1 - pair, pairs, axis=0)
    ordered = jnp.swapaxes(ordered, 0, 1)
    mid_after = pick(after, 2 * pair)
    mid = (
        jnp.exp(pick(even_before, pair) - mid_after)[:, None, None, None]
        * ordered.astype(jnp.float32)
        + jnp.exp(pick(own_level, 2 * pair) - mid_after)[:, None, None, None] * low
    ).astype(jnp.bfloat16)
    mine = jnp.where(first, ordered, mid)
    other = send(jnp.where(first, mid, ordered), "sp", size, lambda k: k ^ 1)
    state = jnp.stack(
        [jnp.where(first, mine, other), jnp.where(first, other, mine)], axis=2
    ).reshape(count, head_width, head_width)

    frame = pick(before, me)
    stabilizer = frame + pick(totals, me) - total
    blocks = jnp.arange(size)[:, None]
    shares = jnp.where(blocks < me, jnp.exp(jnp.minimum(own_level - frame[None], 0.0)), 0.0)
    norm_state = jnp.exp(level - frame)[:, None] * start_normal + jnp.sum(
        shares[..., None] * norms, axis=0
    )

    causal = jnp.tril(jnp.ones((length, length), dtype=bool))
    logits = jnp.where(
        causal,
        cumulative[:, :, None] - cumulative[:, None, :] + gate_in[:, None, :],
        negative_fill,
    )
    carried = cumulative + stabilizer[:, None]
    running_max = jnp.maximum(carried, jnp.max(logits, axis=-1))
    raw = (
        jnp.einsum("ptd,psd->pts", query, key_in, preferred_element_type=jnp.float32) * factor
    )
    scores = raw * jnp.exp(logits - running_max[..., None])
    carry_weight = jnp.exp(carried - running_max) * factor
    inner = jnp.einsum(
        "pts,pse->pte", scores.astype(jnp.bfloat16), value, preferred_element_type=jnp.float32
    )
    denominator = jnp.sum(scores, axis=-1) + carry_weight * jnp.sum(
        query.astype(jnp.float32) * norm_state[:, None, :], axis=-1
    )
    numerator = inner + carry_weight[..., None] * jnp.einsum(
        "ptd,pde->pte", query, state, preferred_element_type=jnp.float32
    )
    return (numerator / jnp.maximum(jnp.abs(denominator), 1.0)[..., None]).astype(jnp.bfloat16)


def on_device(
    queries,
    keys,
    values,
    input_gate,
    forget_gate,
    start_memory,
    start_norm,
    start_level,
    head_gain,
    out_weight,
):
    local_seqs, heads, tokens_here, head_width = queries.shape
    count = local_seqs * heads
    pieces, width = gather_weight(out_weight, lax.axis_size("dp"))

    def to_items(tensor):
        return tensor.reshape((count,) + tensor.shape[2:])

    hidden = cell(
        to_items(queries),
        to_items(keys),
        to_items(values),
        to_items(input_gate),
        to_items(forget_gate),
        to_items(start_memory),
        to_items(start_norm),
        start_level.reshape(count),
        lax.axis_size("sp"),
    ).reshape(local_seqs, heads, tokens_here, head_width)
    normed = (hidden.astype(jnp.float32) * head_gain[:, None, :]).astype(jnp.bfloat16)
    flat = jnp.swapaxes(normed, 1, 2).reshape(local_seqs, tokens_here, heads * head_width)
    mixed = jnp.zeros(
        (local_seqs, tokens_here, out_weight.shape[1] * lax.axis_size("dp")), jnp.bfloat16
    )
    for block, chunk, piece in pieces:
        part = jnp.einsum("stf,fc->stc", flat, piece, preferred_element_type=jnp.float32)
        mixed = lax.dynamic_update_slice(
            mixed,
            part.astype(jnp.bfloat16),
            (0, 0, block * out_weight.shape[1] + chunk * width),
        )
    return mixed


def solution(mesh):
    in_specs = (
        P("dp", None, "sp", None),
        P("dp", None, "sp", None),
        P("dp", None, "sp", None),
        P("dp", None, "sp"),
        P("dp", None, "sp"),
        P("dp", None, "sp", None),
        P("dp", None, "sp"),
        P("dp", None),
        P(),
        P(None, "dp"),
    )
    out_specs = P("dp", "sp", None)

    return jax.shard_map(on_device, mesh=mesh, in_specs=in_specs, out_specs=out_specs, check_vma=False)
```
